256 devices in a mesh: grp: 2 (over y), ra: 16 (over z), cb: 8 (over x, core).
Axes of the slice: x: 4, y: 2, z: 16, core: 2. Of those that a mesh axis runs over, the one named last changes fastest.
The devices are a block of a 4x16x16 slice.
Arguments:
- tokens: bfloat16 [2048, 4096], P('grp', 'ra'), parts along dimension 0, may hold values from -20 to 20
- norm_gain: float32 [2, 4096], P(None, 'ra'), may hold values from 0.1 to 1.9
- up_weight: float32 [2, 4096, 16384], P(None, 'ra', 'cb'), may hold values from -0.125 to 0.125
- up_scale: float32 [2, 16384], P(None, 'cb'), may hold values from 0.1 to 1.9
- down_weight: float32 [2, 16384, 4096], P(None, 'cb', 'ra'), may hold values from -0.046875 to 0.046875
- down_scale: float32 [2, 4096], P(None, 'ra'), may hold values from 0.1 to 1.9
Outputs:
- mixed: bfloat16 [2048, 4096], P('grp', 'ra'), parts along dimension 0
The draws below stay inside these ranges and needn't reach their ends.
There are 2 independent parts, one for each index of `grp`. The reference program is written for one: setup_inputs(seed, part) draws one part's arguments, and reference() takes and returns one part's arrays. A program takes and returns all parts, laid end to end along the dimension named above; an argument that names none is the same for every part. Nothing has to cross between parts.
All inputs are finite; a program needn't handle non-finite values.
Results may differ from the reference program's by a relative error of at most 0.023.
Values may be sent and summed in bfloat16 or wider, within the bound.
No kernel may reach another device: no remote copies, remote signals or barrier semaphores. Data moves between devices by JAX's collectives and lax.ppermute only.
A program may use at most 128 MiB of HBM per device.

```python
import math
import jax
import jax.numpy as jnp
from jax import lax

D = 4096
FF = 16384
LAYERS = 2
TOKENS = 1024


def draw_tokens(key, part):
    first = jax.random.fold_in(key, 11)
    second = jax.random.fold_in(key, 23)
    groups = D // 128
    column_scale = jnp.exp(jax.random.uniform(second, (groups,), jnp.float32, math.log(0.3), math.log(3.0)))
    column_scale = jnp.repeat(column_scale, D // groups)
    values = jnp.clip(jax.random.normal(first, (TOKENS, D), jnp.float32), -6.0, 6.0)
    return jnp.clip(values * column_scale[None, :], -20.0, 20.0).astype(jnp.bfloat16)


def strengthened(array, key, source, target, parts, factor):
    def block_of(dim):
        return (jnp.arange(array.shape[dim]) // (array.shape[dim] // parts)).reshape((-1,) + (1,) * (array.ndim - 1 - dim))

    near = jax.random.permutation(key, parts)[block_of(target)]
    other_side = (block_of(target) + parts // 2) % parts
    return jnp.where((block_of(source) == near) | (block_of(source) == other_side), factor * array, array)


def block_levels(key, shape, shards, least, largest):
    def one(dim, shards_of):
        heights = jax.random.uniform(jax.random.fold_in(jax.random.fold_in(key, 6), dim), (shards_of,), jnp.float32, least / len(shards), largest / len(shards))
        return jnp.repeat(jnp.exp(heights), shape[dim] // shards_of).reshape((-1,) + (1,) * (len(shape) - dim - 1))

    level = one(*shards[0])
    for cut in shards[1:]:
        level = level * one(*cut)
    return level


def gaussian(stream_key, dims, spread, most, pieces=(), kind=jnp.bfloat16):
    entries = jax.random.normal(stream_key, dims, jnp.float32) * spread
    if len(pieces) > 0:
        entries = block_levels(stream_key, dims, pieces, -0.22, 0.18) * entries
    return jnp.clip(entries, min=-most, max=most).astype(kind)


def noise_with(own_key, shape, spread, bound, pieces, heavy, dtype=jnp.bfloat16):
    array = spread * jax.random.normal(own_key, shape, jnp.float32)
    if pieces:
        array = array * block_levels(own_key, shape, pieces, -0.22, 0.18)
    return jnp.clip(strengthened(array, jax.random.fold_in(own_key, 3), *heavy), -bound, bound).astype(dtype)


def setup_inputs(seed: int = 0, part: int = 0) -> dict:
    seeds = jax.random.split(jax.random.key(seed), 7)
    part_splits = jax.random.split(jax.random.fold_in(seeds[6], part), 7)
    tokens = draw_tokens(jax.random.fold_in(jax.random.fold_in(seeds[6], part), 71), part)
    norm_gain = jnp.clip(1.0 + 0.18 * jax.random.normal(seeds[1], (LAYERS, D), jnp.float32), 0.1, 1.9)
    up_weight = noise_with(seeds[2], (LAYERS, D, FF), D ** -0.5, 0.125, ((1, 16), (2, 8)), (1, 2, 16, 2.0), jnp.float32)
    up_scale = jnp.clip(1.0 + 0.18 * jax.random.normal(seeds[3], (LAYERS, FF), jnp.float32), 0.1, 1.9)
    down_weight = gaussian(seeds[4], (LAYERS, FF, D), FF ** -0.5, 0.046875, ((1, 8), (2, 16)), jnp.float32)
    down_scale = jnp.clip(1.0 + 0.18 * jax.random.normal(seeds[5], (LAYERS, D), jnp.float32), 0.1, 1.9)
    return dict(tokens=tokens, norm_gain=norm_gain, up_weight=up_weight, up_scale=up_scale, down_weight=down_weight, down_scale=down_scale)


epsilon = 1e-06
residual_keep = 0.5

def reference(tokens, norm_gain, up_weight, up_scale, down_weight, down_scale):
    current = tokens
    for sublayer in range(LAYERS):
        widened = current.astype(jnp.float32)
        mean_square = lax.optimization_barrier(jnp.mean(widened * widened, axis=1, keepdims=True))
        scaled = (widened * norm_gain[sublayer]).astype(jnp.bfloat16)
        upward = jnp.dot(scaled, up_weight[sublayer].astype(jnp.bfloat16), preferred_element_type=jnp.float32)
        active = jnp.maximum(upward * lax.rsqrt(mean_square + epsilon) * up_scale[sublayer], 0.0)
        hidden = (active * active).astype(jnp.bfloat16)
        downward = jnp.dot(hidden, down_weight[sublayer].astype(jnp.bfloat16), preferred_element_type=jnp.float32)
        current = (residual_keep * widened + downward * down_scale[sublayer]).astype(jnp.bfloat16)
    return current
```

```python
import jax
import jax.numpy as jnp
from jax import lax
from jax.sharding import PartitionSpec as P

epsilon = 1e-06
residual_keep = 0.5
CHUNKS = 2
SPARE = 128


def ring(axis):
    count = lax.axis_size(axis)
    ahead = [(i, (i + 1) % count) for i in range(count)]
    behind = [(i, (i - 1) % count) for i in range(count)]
    return count, ahead, behind


def turned(blocks, start):
    count = blocks.shape[0]
    return lax.dynamic_slice_in_dim(jnp.concatenate([blocks, blocks], 0), start % count, count, 0)


def exact_pieces(value):
    pieces = []
    for _ in range(3):
        piece = lax.reduce_precision(value, 8, 7)
        pieces.append(piece)
        value = value - piece
    return jnp.concatenate(pieces, axis=1)


def reduce_round(blocks, axis, far_ahead):
    count, ahead, behind = ring(axis)
    half = count // 2
    up = [half + k for k in range(half - (0 if far_ahead else 1), 0, -1)]
    down = [half - k for k in range(half - (1 if far_ahead else 0), 0, -1)]
    flows = [None, None]
    for step in range(half):
        for side, (places, way) in enumerate(((up, ahead), (down, behind))):
            at = step - (half - len(places))
            if at < 0:
                continue
            mine = blocks[places[at] % count]
            flows[side] = lax.ppermute(mine if at == 0 else flows[side] + mine, axis, way)
        if None not in flows:
            flows = list(lax.optimization_barrier(tuple(flows)))
    wide = [m.astype(jnp.float32) for m in flows]
    return blocks[half].astype(jnp.float32) + wide[0] + wide[1]


def gather_round(own, axis, far_ahead):
    count, ahead, behind = ring(axis)
    half = count // 2
    got = {half: own}
    flows = [own, own]
    lengths = (half - (0 if far_ahead else 1), half - (1 if far_ahead else 0))
    for step in range(1, half + 1):
        for side, (way, sign) in enumerate(((ahead, -1), (behind, 1))):
            if step <= lengths[side]:
                flows[side] = lax.ppermute(flows[side], axis, way)
                got[(half + sign * step) % count] = flows[side]
        flows = list(lax.optimization_barrier(tuple(flows)))
        for side, sign in enumerate((-1, 1)):
            if step <= lengths[side]:
                got[(half + sign * step) % count] = flows[side]
    return jnp.concatenate([got[j] for j in range(count)], 0)


def shards(tokens, norm_gain, up_weight, up_scale, down_weight, down_scale):
    count = lax.axis_size("ra")
    place = lax.axis_index("ra")
    width = tokens.shape[1] * count
    hidden_width = up_weight.shape[2]
    per_chunk = tokens.shape[0] // CHUNKS
    rows = per_chunk // count
    half = count // 2
    current = []
    for c in range(CHUNKS):
        part = tokens[c * per_chunk : (c + 1) * per_chunk].reshape(count, rows, -1)
        current.append(turned(part, place + half).reshape(per_chunk, -1))
    lanes = jnp.arange(SPARE)[None, :]
    for sublayer in range(up_weight.shape[0]):
        up_matrix = up_weight[sublayer].astype(jnp.bfloat16)
        down_matrix = down_weight[sublayer].astype(jnp.bfloat16)
        owned = []
        for c in range(CHUNKS):
            widened = current[c].astype(jnp.float32)
            squares = jnp.sum(widened * widened, axis=1, keepdims=True)
            pieces = exact_pieces(squares)
            spare = jnp.zeros((per_chunk, SPARE), jnp.float32)
            for k in range(3):
                spare = jnp.where(lanes == 3 * place + k, pieces[:, k : k + 1], spare)
            scaled = (widened * norm_gain[sublayer]).astype(jnp.bfloat16)
            upward = jnp.dot(scaled, up_matrix, preferred_element_type=jnp.float32).astype(jnp.bfloat16)
            blocks = jnp.concatenate([upward, spare.astype(jnp.bfloat16)], axis=1).reshape(count, rows, -1)
            owned.append(reduce_round(blocks, "ra", c % 2 == 1))
        gathered = []
        for c in range(CHUNKS):
            total = owned[c]
            squares = jnp.sum(total[:, hidden_width:], axis=1, keepdims=True)
            active = total[:, :hidden_width] * lax.rsqrt(squares / width + epsilon) * up_scale[sublayer]
            active = jnp.maximum(active, 0.0)
            gathered.append(gather_round((active * active).astype(jnp.bfloat16), "ra", c % 2 == 0))
        following = []
        for c in range(CHUNKS):
            downward = jnp.dot(gathered[c], down_matrix, preferred_element_type=jnp.float32)
            parts = lax.all_gather(downward.astype(jnp.bfloat16), "cb")
            summed = parts.astype(jnp.float32).sum(0)
            kept = residual_keep * current[c].astype(jnp.float32)
            following.append((kept + summed * down_scale[sublayer]).astype(jnp.bfloat16))
        current = following
    out = []
    for c in range(CHUNKS):
        out.append(turned(current[c].reshape(count, rows, -1), half - place).reshape(per_chunk, -1))
    return jnp.concatenate(out, 0)


def solution(mesh):
    in_specs = (
        P("grp", "ra"),
        P(None, "ra"),
        P(None, "ra", "cb"),
        P(None, "cb"),
        P(None, "cb", "ra"),
        P(None, "ra"),
    )
    out_specs = P("grp", "ra")
    return jax.shard_map(shards, mesh=mesh, in_specs=in_specs, out_specs=out_specs, check_vma=False)
```

```python
import jax
import jax.numpy as jnp
from jax import lax
from jax.sharding import PartitionSpec as P

epsilon = 1e-06
residual_keep = 0.5
CHUNKS = 2
SPARE = 128


def ring(axis):
    count = lax.axis_size(axis)
    ahead = [(i, (i + 1) % count) for i in range(count)]
    behind = [(i, (i - 1) % count) for i in range(count)]
    return count, ahead, behind


def turned(blocks, start):
    count = blocks.shape[0]
    return lax.dynamic_slice_in_dim(jnp.concatenate([blocks, blocks], 0), start % count, count, 0)


def exact_pieces(value):
    pieces = []
    for _ in range(3):
        piece = lax.reduce_precision(value, 8, 7)
        pieces.append(piece)
        value = value - piece
    return jnp.concatenate(pieces, axis=1)


def reduce_round(blocks, axis, far_ahead):
    count, ahead, behind = ring(axis)
    half = count // 2
    up = [half + k for k in range(half - (0 if far_ahead else 1), 0, -1)]
    down = [half - k for k in range(half - (1 if far_ahead else 0), 0, -1)]
    flows = [None, None]
    for step in range(half):
        for side, (places, way) in enumerate(((up, ahead), (down, behind))):
            at = step - (half - len(places))
            if at < 0:
                continue
            mine = blocks[places[at] % count]
            flows[side] = lax.ppermute(mine if at == 0 else flows[side] + mine, axis, way)
        if None not in flows:
            flows = list(lax.optimization_barrier(tuple(flows)))
    wide = [m.astype(jnp.float32) for m in flows]
    return blocks[half].astype(jnp.float32) + wide[0] + wide[1]


def gather_round(own, axis, far_ahead):
    count, ahead, behind = ring(axis)
    half = count // 2
    got = {half: own}
    flows = [own, own]
    lengths = (half - (0 if far_ahead else 1), half - (1 if far_ahead else 0))
    for step in range(1, half + 1):
        for side, (way, sign) in enumerate(((ahead, -1), (behind, 1))):
            if step <= lengths[side]:
                flows[side] = lax.ppermute(flows[side], axis, way)
                got[(half + sign * step) % count] = flows[side]
        flows = list(lax.optimization_barrier(tuple(flows)))
        for side, sign in enumerate((-1, 1)):
            if step <= lengths[side]:
                got[(half + sign * step) % count] = flows[side]
    return jnp.concatenate([got[j] for j in range(count)], 0)


def shards(tokens, norm_gain, up_weight, up_scale, down_weight, down_scale):
    count = lax.axis_size("ra")
    place = lax.axis_index("ra")
    width = tokens.shape[1] * count
    hidden_width = up_weight.shape[2]
    per_chunk = tokens.shape[0] // CHUNKS
    rows = per_chunk // count
    half = count // 2
    current = []
    for c in range(CHUNKS):
        part = tokens[c * per_chunk : (c + 1) * per_chunk].reshape(count, rows, -1)
        current.append(turned(part, place + half).reshape(per_chunk, -1))
    lanes = jnp.arange(SPARE)[None, :]
    for sublayer in range(up_weight.shape[0]):
        up_matrix = up_weight[sublayer].astype(jnp.bfloat16)
        down_matrix = down_weight[sublayer].astype(jnp.bfloat16)
        owned = []
        for c in range(CHUNKS):
            widened = current[c].astype(jnp.float32)
            squares = jnp.sum(widened * widened, axis=1, keepdims=True)
            pieces = exact_pieces(squares)
            spare = jnp.zeros((per_chunk, SPARE), jnp.float32)
            for k in range(3):
                spare = jnp.where(lanes == 3 * place + k, pieces[:, k : k + 1], spare)
            scaled = (widened * norm_gain[sublayer]).astype(jnp.bfloat16)
            upward = jnp.dot(scaled, up_matrix, preferred_element_type=jnp.float32).astype(jnp.bfloat16)
            blocks = jnp.concatenate([upward, spare.astype(jnp.bfloat16)], axis=1).reshape(count, rows, -1)
            owned.append(reduce_round(blocks, "ra", c % 2 == 1))
        gathered = []
        for c in range(CHUNKS):
            total = owned[c]
            squares = jnp.sum(total[:, hidden_width:], axis=1, keepdims=True)
            active = total[:, :hidden_width] * lax.rsqrt(squares / width + epsilon) * up_scale[sublayer]
            active = jnp.maximum(active, 0.0)
            gathered.append(gather_round((active * active).astype(jnp.bfloat16), "ra", c % 2 == 0))
        downward = jnp.concatenate(
            [jnp.dot(g, down_matrix, preferred_element_type=jnp.float32).astype(jnp.bfloat16) for g in gathered], 0
        )
        sharers = lax.axis_size("cb")
        share = downward.shape[0] // sharers
        parts = lax.all_to_all(downward.reshape(sharers, share, -1), "cb", 0, 0, tiled=True)
        summed = parts.astype(jnp.float32).sum(0)
        before = jnp.concatenate(current, 0)
        kept = lax.dynamic_slice_in_dim(before, lax.axis_index("cb") * share, share, 0).astype(jnp.float32)
        piece = (residual_keep * kept + summed * down_scale[sublayer]).astype(jnp.bfloat16)
        copies = jnp.broadcast_to(piece[None], (sharers, *piece.shape))
        after = lax.all_to_all(copies, "cb", 0, 0, tiled=True).reshape(downward.shape)
        current = [after[c * per_chunk : (c + 1) * per_chunk] for c in range(CHUNKS)]
    out = []
    for c in range(CHUNKS):
        out.append(turned(current[c].reshape(count, rows, -1), half - place).reshape(per_chunk, -1))
    return jnp.concatenate(out, 0)


def solution(mesh):
    in_specs = (
        P("grp", "ra"),
        P(None, "ra"),
        P(None, "ra", "cb"),
        P(None, "cb"),
        P(None, "cb", "ra"),
        P(None, "ra"),
    )
    out_specs = P("grp", "ra")
    return jax.shard_map(shards, mesh=mesh, in_specs=in_specs, out_specs=out_specs, check_vma=False)
```
